32 devices in a mesh: vp: 8 (over z, x), dp: 4 (over y, core).
Axes of the slice: x: 2, y: 2, z: 4, core: 2. Of those that a mesh axis runs over, the one named last changes fastest.
Arguments:
- stream: bfloat16 [8192, 2048], P(('dp', 'vp')), may hold values from -6 to 6
- norm_gain: float32 [2048], replicated, may hold values from 0.1 to 1.9
- vocab_matrix: bfloat16 [2048, 16384], P(None, 'vp'), may hold values from -0.3125 to 0.3125
- column_bias: float32 [16384], P('vp'), may hold values from -3 to 100
- targets: int32 [8192], P('dp'), may hold values from 0 to 16383
Outputs:
- losses: float32 [8192], P(('dp', 'vp'))
- normin_grad: float32 [8192, 2048], P(('dp', 'vp'))
- vocab_grad: float32 [2048, 16384], P('dp', 'vp')
The draws below stay inside these ranges and needn't reach their ends.
All inputs are finite; a program needn't handle non-finite values.
Results may differ from the reference program's by a relative error of at most 0.0031.
Values may be sent and summed in bfloat16 or wider, within the bound.
A program may use at most 128 MiB of HBM per device.

```python
import math
import jax
import jax.numpy as jnp
import numpy as np
from jax import lax

D = 2048
V = 16384
TOKENS = 8192
BLOCK_ROWS = 512


def draw_column_bias(key, part):
    columns = jnp.arange(V)
    pattern = 1.2 * jnp.sin(2.3 * (columns * 16 // V).astype(jnp.float32) + 0.4)
    baseline = jnp.clip(jax.random.normal(key, (V,), jnp.float32), -3.0, 3.0) * 0.6
    return baseline + pattern


def plant(array, rng, least, top_value):
    longest = array.shape.index(max(array.shape))
    spots = []
    for shift in (0, 1):
        where = [jax.random.randint(jax.random.fold_in(rng, axis), (), 0, length) for axis, length in enumerate(array.shape)]
        where[longest] = (where[longest] + shift) % array.shape[longest]
        spots.append(tuple(where))
    return array.at[spots[0]].set(least).at[spots[1]].set(top_value)


def level_of(key, shape, cuts, least, largest):
    loudness, own = 1.0, jax.random.fold_in(key, 6)
    for axis_at, shards_of in cuts:
        heights = jnp.exp(jax.random.uniform(jax.random.fold_in(own, axis_at), (shards_of,), jnp.float32, least / len(cuts), largest / len(cuts)))
        loudness = loudness * jnp.repeat(heights, shape[axis_at] // shards_of).reshape([-1 if axis == axis_at else 1 for axis in range(len(shape))])
    return loudness


def rank_bounds(amount, slope):
    loads = [(1 << 20) // math.isqrt(standing ** slope) + 1 for standing in range(1, amount + 1)]
    spread = 1 + sum(loads) // (1 << 30)
    return np.cumsum(np.array([max(1, weight // spread) for weight in loads]))


def skewed_ids(key, shape, number_of, skew):
    grid = rank_bounds(number_of, skew)
    lot = jax.random.randint(jax.random.fold_in(key, 1), shape, 0, int(grid[number_of - 1]))
    grade = jnp.searchsorted(jnp.asarray(grid, jnp.int32), lot, side="right")
    return jax.random.permutation(jax.random.fold_in(key, 2), number_of)[grade].astype(jnp.int32)


def bell_draw(rng, extent, scale, reach, pieces=(), kind=jnp.bfloat16):
    loudness = level_of(rng, extent, pieces, -0.22, 0.18) if pieces else 1.0
    result = jax.random.normal(rng, extent, jnp.float32) * scale * loudness
    return jnp.minimum(jnp.maximum(result, -reach), reach).astype(kind)


def setup_inputs(seed: int = 0) -> dict:
    keys = jax.random.split(jax.random.key(seed), 6)
    return {
        "stream": bell_draw(keys[0], (TOKENS, D), 1.0, 6.0, ((0, 32),)),
        "norm_gain": jnp.clip(1.0 + 0.18 * jax.random.normal(keys[1], (D,), jnp.float32), 0.1, 1.9),
        "vocab_matrix": bell_draw(keys[2], (D, V), (D // 6) ** -0.5, 0.3125, ((1, 8),)),
        "column_bias": draw_column_bias(jax.random.fold_in(keys[5], 71), 0),
        "targets": plant(skewed_ids(keys[4], (TOKENS,), V, 2), jax.random.fold_in(keys[4], 3), 0, V - 1).astype(jnp.int32),
    }


PENALTY = 0.001
EPSILON = 1e-06

def reference(stream, norm_gain, vocab_matrix, column_bias, targets):
    normin = stream.astype(jnp.float32)
    inverse = lax.rsqrt(lax.optimization_barrier(jnp.mean(normin * normin, axis=1, keepdims=True)) + EPSILON)
    normed = (normin * inverse * norm_gain).astype(jnp.bfloat16)
    num_blocks = TOKENS // BLOCK_ROWS
    columns = jnp.arange(vocab_matrix.shape[1], dtype=jnp.int32)

    def advance(running, block_index):
        start_row = (block_index * BLOCK_ROWS).astype(jnp.int32)
        block_normed = lax.dynamic_slice_in_dim(normed, start_row, BLOCK_ROWS, 0)
        wanted = lax.dynamic_slice_in_dim(targets, start_row, BLOCK_ROWS, 0)
        scores = jnp.dot(block_normed, vocab_matrix, preferred_element_type=jnp.float32) + column_bias
        row_max = lax.optimization_barrier(jnp.max(scores, axis=1, keepdims=True))
        row_sum = lax.optimization_barrier(jnp.sum(jnp.exp(scores - row_max), axis=1, keepdims=True))
        log_total = row_max + jnp.log(row_sum)
        is_target = columns[None, :] == wanted[:, None]
        picked = lax.optimization_barrier(jnp.sum(jnp.where(is_target, scores, 0.0), axis=1))
        flat_total = log_total[:, 0]
        block_loss = flat_total - picked + PENALTY * flat_total * flat_total
        factor = 1.0 + 2.0 * PENALTY * log_total
        weight = (jnp.exp(scores - log_total) * factor - is_target.astype(jnp.float32)).astype(jnp.bfloat16)
        rows_grad = lax.dot_general(weight, vocab_matrix, (((1,), (1,)), ((), ())), preferred_element_type=jnp.float32)
        running = running + lax.dot_general(block_normed, weight, (((0,), (0,)), ((), ())), preferred_element_type=jnp.float32)
        return (running, (block_loss, rows_grad))
    zeros_grad = jnp.zeros((vocab_matrix.shape[0], vocab_matrix.shape[1]), jnp.float32)
    vocab_grad, (losses, rows_grad) = lax.scan(advance, zeros_grad, jnp.arange(num_blocks, dtype=jnp.int32))
    losses = losses.reshape(-1)
    rows_grad = rows_grad.reshape(-1, vocab_matrix.shape[0])
    scaled = rows_grad * norm_gain
    projected = lax.optimization_barrier(jnp.mean(scaled * normin, axis=1, keepdims=True))
    normin_grad = inverse * (scaled - normin * inverse * inverse * projected)
    return (losses, normin_grad, vocab_grad)
```

```python
import jax
import jax.numpy as jnp
from jax import lax
from jax.sharding import PartitionSpec as P

PENALTY = 0.001
EPSILON = 1e-06


def minor_size(count):
    return 1 << ((count.bit_length() - 1) // 2)


class Ring:
    def __init__(self, axis, outer, inner, over_outer):
        self.axis, self.outer, self.inner, self.over_outer = axis, outer, inner, over_outer
        self.size = outer if over_outer else inner

    def shift(self, value, by):
        pairs = []
        for hi in range(self.outer):
            for lo in range(self.inner):
                to_hi, to_lo = (
                    ((hi + by) % self.outer, lo) if self.over_outer else (hi, (lo + by) % self.inner)
                )
                pairs.append((hi * self.inner + lo, to_hi * self.inner + to_lo))
        return lax.ppermute(value, self.axis, pairs)

    def gather(self, block):
        n = self.size
        blocks = {0: block}
        if n == 1:
            return blocks
        if n == 2:
            blocks[1] = self.shift(block, 1)
            return blocks
        before, after = block, block
        for step in range(1, n // 2):
            before, after = self.shift(before, 1), self.shift(after, -1)
            blocks[n - step], blocks[step] = before, after
        half = block.shape[0] // 2
        blocks[n // 2] = jnp.concatenate(
            [self.shift(before[:half], 1), self.shift(after[half:], -1)], axis=0
        )
        return blocks

    def scatter(self, blocks):
        n = self.size

        def sent(value, by):
            return self.shift(value.astype(jnp.bfloat16), by).astype(jnp.float32)

        if n == 1:
            return blocks[0]
        if n == 2:
            return blocks[0] + sent(blocks[1], 1)
        far = blocks[n // 2]
        half = far.shape[0] // 2
        up, down = sent(far[:half], 1), sent(far[half:], -1)
        plus, minus = blocks[n // 2 - 1], blocks[n // 2 + 1]
        plus = jnp.concatenate([plus[:half] + up, plus[half:]], axis=0)
        minus = jnp.concatenate([minus[:half], minus[half:] + down], axis=0)
        for step in range(n // 2 - 1, 0, -1):
            up, down = sent(plus, 1), sent(minus, -1)
            if step > 1:
                plus, minus = blocks[step - 1] + up, blocks[n - step + 1] + down
        return blocks[0] + up + down


def per_device(vp, dp, stream, norm_gain, vocab_matrix, column_bias, targets):
    inner = minor_size(vp)
    outer = vp // inner
    z_ring = Ring("vp", outer, inner, True)
    x_ring = Ring("vp", outer, inner, False)
    me = lax.axis_index("vp")
    my_z, my_x = me // inner, me % inner
    rows = stream.shape[0]
    col_count = vocab_matrix.shape[1]

    def norm_of(block):
        normin = block.astype(jnp.float32)
        inverse = lax.rsqrt(jnp.mean(normin * normin, axis=1, keepdims=True) + EPSILON)
        return normin, inverse, (normin * inverse * norm_gain).astype(jnp.bfloat16)

    normin, inverse, mine = norm_of(stream)
    places = {}
    for dz, block in z_ring.gather(mine).items():
        for dx, piece in x_ring.gather(block).items():
            places[dz, dx] = piece
    keys = sorted(places, key=lambda key: (min(key[0], outer - key[0]), key[1]))
    owners = jnp.stack([((my_z + dz) % outer) * inner + (my_x + dx) % inner for dz, dx in keys])
    columns = jnp.arange(col_count, dtype=jnp.int32)
    wanted = jnp.take(targets.reshape(vp, rows) - me * col_count, owners, axis=0)
    scores, stats = [], []
    for at, key in enumerate(keys):
        score = jnp.dot(places[key], vocab_matrix, preferred_element_type=jnp.float32) + column_bias
        hit = columns[None, :] == wanted[at][:, None]
        top = jnp.max(score, axis=1)
        total = jnp.sum(jnp.exp(score - top[:, None]), axis=1)
        pick = jnp.sum(jnp.where(hit, score, 0.0), axis=1)
        scores.append(score)
        stats.append(jnp.stack([top, total, pick]))
    back = jnp.argsort(owners)
    local = jnp.take(jnp.stack(stats), back, axis=0)
    every = lax.all_gather(local, "vp", axis=0)
    tops, totals, picks = every[:, :, 0], every[:, :, 1], every[:, :, 2]
    top = jnp.max(tops, axis=0)
    log_total = top + jnp.log(jnp.sum(totals * jnp.exp(tops - top[None]), axis=0))
    picked = jnp.sum(picks, axis=0)
    losses_all = log_total - picked + PENALTY * log_total * log_total
    losses = lax.dynamic_index_in_dim(losses_all, me, 0, keepdims=False)
    logs = jnp.take(log_total, owners, axis=0)

    weights, grads = {}, {}
    for at, key in enumerate(keys):
        span = logs[at][:, None]
        hit = columns[None, :] == wanted[at][:, None]
        weights[key] = (
            jnp.exp(scores[at] - span) * (1.0 + 2.0 * PENALTY * span) - hit.astype(jnp.float32)
        ).astype(jnp.bfloat16)
    for key in keys:
        grads[key] = lax.dot_general(
            weights[key], vocab_matrix, (((1,), (1,)), ((), ())), preferred_element_type=jnp.float32
        )
    by_z = {dz: x_ring.scatter({dx: grads[dz, dx] for dx in range(inner)}) for dz in range(outer)}
    rows_grad = z_ring.scatter(by_z)
    scaled = rows_grad * norm_gain
    projected = jnp.mean(scaled * normin, axis=1, keepdims=True)
    normin_grad = inverse * (scaled - normin * inverse * inverse * projected)

    local_grad = lax.dot_general(
        jnp.concatenate([places[key] for key in keys], axis=0),
        jnp.concatenate([weights[key] for key in keys], axis=0),
        (((0,), (0,)), ((), ())),
        preferred_element_type=jnp.float32,
    )
    core_ring = Ring("dp", dp // 2, 2, False)
    y_ring = Ring("dp", dp // 2, 2, True)
    my_dp = lax.axis_index("dp")
    parts = local_grad.reshape(dp // 2, 2, -1, col_count)
    core = my_dp % 2
    kept = lax.dynamic_index_in_dim(parts, core, 1, keepdims=False)
    other = lax.dynamic_index_in_dim(parts, 1 - core, 1, keepdims=False)
    halves = core_ring.scatter({0: kept, 1: other})
    vocab_grad = y_ring.scatter(
        {
            dy: lax.dynamic_index_in_dim(halves, (my_dp // 2 + dy) % (dp // 2), 0, keepdims=False)
            for dy in range(dp // 2)
        }
    )
    return (losses, normin_grad, vocab_grad)


def solution(mesh):
    vp, dp = mesh.shape["vp"], mesh.shape["dp"]
    placed = (P(("dp", "vp"), None), P(), P(None, "vp"), P("vp"), P("dp"))

    def whole(*args):
        return per_device(vp, dp, *args)

    return jax.shard_map(
        whole,
        mesh=mesh,
        in_specs=placed,
        out_specs=(P(("dp", "vp")), P(("dp", "vp"), None), P("dp", "vp")),
        check_vma=False,
    )
```

```python
import jax
import jax.numpy as jnp
from jax import lax
from jax.sharding import PartitionSpec as P

PENALTY = 0.001
EPSILON = 1e-06


def minor_size(count):
    return 1 << ((count.bit_length() - 1) // 2)


class Ring:
    def __init__(self, axis, outer, inner, over_outer):
        self.axis, self.outer, self.inner, self.over_outer = axis, outer, inner, over_outer
        self.size = outer if over_outer else inner

    def shift(self, value, by):
        pairs = []
        for hi in range(self.outer):
            for lo in range(self.inner):
                to_hi, to_lo = (
                    ((hi + by) % self.outer, lo) if self.over_outer else (hi, (lo + by) % self.inner)
                )
                pairs.append((hi * self.inner + lo, to_hi * self.inner + to_lo))
        return lax.ppermute(value, self.axis, pairs)

    def gather(self, block):
        n = self.size
        blocks = {0: block}
        if n == 1:
            return blocks
        if n == 2:
            blocks[1] = self.shift(block, 1)
            return blocks
        before, after = block, block
        for step in range(1, n // 2):
            before, after = self.shift(before, 1), self.shift(after, -1)
            blocks[n - step], blocks[step] = before, after
        half = block.shape[0] // 2
        blocks[n // 2] = jnp.concatenate(
            [self.shift(before[:half], 1), self.shift(after[half:], -1)], axis=0
        )
        return blocks

    def scatter(self, blocks):
        n = self.size

        def sent(value, by):
            return self.shift(value.astype(jnp.bfloat16), by).astype(jnp.float32)

        if n == 1:
            return blocks[0]
        if n == 2:
            return blocks[0] + sent(blocks[1], 1)
        far = blocks[n // 2]
        half = far.shape[0] // 2
        up, down = sent(far[:half], 1), sent(far[half:], -1)
        plus, minus = blocks[n // 2 - 1], blocks[n // 2 + 1]
        plus = jnp.concatenate([plus[:half] + up, plus[half:]], axis=0)
        minus = jnp.concatenate([minus[:half], minus[half:] + down], axis=0)
        for step in range(n // 2 - 1, 0, -1):
            up, down = sent(plus, 1), sent(minus, -1)
            if step > 1:
                plus, minus = blocks[step - 1] + up, blocks[n - step + 1] + down
        return blocks[0] + up + down


def per_device(vp, dp, stream, norm_gain, vocab_matrix, column_bias, targets):
    inner = minor_size(vp)
    outer = vp // inner
    z_ring = Ring("vp", outer, inner, True)
    x_ring = Ring("vp", outer, inner, False)
    me = lax.axis_index("vp")
    my_z, my_x = me // inner, me % inner
    rows = stream.shape[0]
    col_count = vocab_matrix.shape[1]

    def norm_of(block):
        normin = block.astype(jnp.float32)
        inverse = lax.rsqrt(jnp.mean(normin * normin, axis=1, keepdims=True) + EPSILON)
        return normin, inverse, (normin * inverse * norm_gain).astype(jnp.bfloat16)

    normin, inverse, mine = norm_of(stream)
    places = {}
    for dz, block in z_ring.gather(mine).items():
        for dx, piece in x_ring.gather(block).items():
            places[dz, dx] = piece
    keys = sorted(places, key=lambda key: (min(key[0], outer - key[0]), key[1]))
    owners = jnp.stack([((my_z + dz) % outer) * inner + (my_x + dx) % inner for dz, dx in keys])
    columns = jnp.arange(col_count, dtype=jnp.int32)
    wanted = jnp.take(targets.reshape(vp, rows) - me * col_count, owners, axis=0)
    scores, stats = [], []
    for at, key in enumerate(keys):
        score = jnp.dot(places[key], vocab_matrix, preferred_element_type=jnp.float32) + column_bias
        hit = columns[None, :] == wanted[at][:, None]
        top = jnp.max(score, axis=1)
        total = jnp.sum(jnp.exp(score - top[:, None]), axis=1)
        pick = jnp.sum(jnp.where(hit, score, 0.0), axis=1)
        scores.append(score)
        stats.append(jnp.stack([top, total, pick]))
    back = jnp.argsort(owners)
    local = jnp.take(jnp.stack(stats), back, axis=0)
    top, total, picked = local[:, 0], local[:, 1], local[:, 2]
    for ring in (x_ring, z_ring):
        held = jnp.stack([top, total, picked])
        pieces = [held] + [ring.shift(held, by) for by in range(1, ring.size)]
        top = pieces[0][0]
        for piece in pieces[1:]:
            top = jnp.maximum(top, piece[0])
        total = sum(piece[1] * jnp.exp(piece[0] - top) for piece in pieces)
        picked = sum(piece[2] for piece in pieces)
    log_total = top + jnp.log(total)
    losses_all = log_total - picked + PENALTY * log_total * log_total
    losses = lax.dynamic_index_in_dim(losses_all, me, 0, keepdims=False)
    logs = jnp.take(log_total, owners, axis=0)

    weights, grads = {}, {}
    for at, key in enumerate(keys):
        span = logs[at][:, None]
        hit = columns[None, :] == wanted[at][:, None]
        weights[key] = (
            jnp.exp(scores[at] - span) * (1.0 + 2.0 * PENALTY * span) - hit.astype(jnp.float32)
        ).astype(jnp.bfloat16)
    def grad_of(key):
        return lax.dot_general(
            weights[key], vocab_matrix, (((1,), (1,)), ((), ())), preferred_element_type=jnp.float32
        )

    token = None
    for key in sorted((k for k in keys if k[1]), key=lambda k: (-min(k[0], outer - k[0]), k)):
        if token is not None:
            weights[key], token = lax.optimization_barrier((weights[key], token))
        token = grad_of(key).astype(jnp.bfloat16)
        grads[key] = token.astype(jnp.float32) if inner == 2 else grad_of(key)
    for key in keys:
        if not key[1]:
            grads[key] = grad_of(key)
    by_z = {dz: x_ring.scatter({dx: grads[dz, dx] for dx in range(inner)}) for dz in range(outer)}
    rows_grad = z_ring.scatter(by_z)
    scaled = rows_grad * norm_gain
    projected = jnp.mean(scaled * normin, axis=1, keepdims=True)
    normin_grad = inverse * (scaled - normin * inverse * inverse * projected)

    local_grad = lax.dot_general(
        jnp.concatenate([places[key] for key in keys], axis=0),
        jnp.concatenate([weights[key] for key in keys], axis=0),
        (((0,), (0,)), ((), ())),
        preferred_element_type=jnp.float32,
    )
    core_ring = Ring("dp", dp // 2, 2, False)
    y_ring = Ring("dp", dp // 2, 2, True)
    my_dp = lax.axis_index("dp")
    parts = local_grad.reshape(dp // 2, 2, -1, col_count)
    core = my_dp % 2
    kept = lax.dynamic_index_in_dim(parts, core, 1, keepdims=False)
    other = lax.dynamic_index_in_dim(parts, 1 - core, 1, keepdims=False)
    halves = core_ring.scatter({0: kept, 1: other})
    vocab_grad = y_ring.scatter(
        {
            dy: lax.dynamic_index_in_dim(halves, (my_dp // 2 + dy) % (dp // 2), 0, keepdims=False)
            for dy in range(dp // 2)
        }
    )
    return (losses, normin_grad, vocab_grad)


def solution(mesh):
    vp, dp = mesh.shape["vp"], mesh.shape["dp"]
    placed = (P(("dp", "vp"), None), P(), P(None, "vp"), P("vp"), P("dp"))

    def whole(*args):
        return per_device(vp, dp, *args)

    return jax.shard_map(
        whole,
        mesh=mesh,
        in_specs=placed,
        out_specs=(P(("dp", "vp")), P(("dp", "vp"), None), P("dp", "vp")),
        check_vma=False,
    )
```
